32 devices in a mesh: ep: 8 (over z, y), tp: 4 (over x, core).
Axes of the slice: x: 2, y: 2, z: 4, core: 2. Of those that a mesh axis runs over, the one named last changes fastest.
Arguments:
- tokens: bfloat16 [6144, 2048], P('ep', 'tp')
- norm_gain: float32 [2048], P('tp'), may hold values from 0.1 to 1.9
- routing: int32 [6144, 2], P('ep'), may hold values from 0 to 7, as said below
- route_weight: float32 [6144, 2], P('ep'), may hold values from 0.2 to 1
- w_gate: bfloat16 [8, 2048, 512], P('ep', 'tp'), may hold values from -0.125 to 0.125
- w_up: bfloat16 [8, 2048, 512], P('ep', 'tp'), may hold values from -0.125 to 0.125
- w_down: bfloat16 [8, 512, 2048], P('ep', None, 'tp'), may hold values from -0.25 to 0.25
- w_branch_in: bfloat16 [2048, 1024], P('ep', 'tp'), may hold values from -0.125 to 0.125
- w_branch_out: bfloat16 [1024, 2048], P('tp', 'ep'), may hold values from -0.1875 to 0.1875
- branch_gate: float32 [2048], P('tp'), may hold values from -3 to 3
Outputs:
- mixed: bfloat16 [6144, 2048], P('ep', 'tp')
The draws below stay inside these ranges and needn't reach their ends.
Inputs may be any that keep to these rules, and one draw needn't show every extreme that they name: `routing`: each row names two different experts of the same group; expert e belongs to group e // 2. Among the rows of one device (aligned blocks of 768 rows) no expert is named more than 384 times, and in every block all experts of one group are named exactly 384 times.
All inputs are finite; a program needn't handle non-finite values.
Results may differ from the reference program's by a relative error of at most 0.0069.
Values may be sent and summed in bfloat16 or wider, within the bound.
No kernel may reach another device: no remote copies, remote signals or barrier semaphores. Data moves between devices by JAX's collectives and lax.ppermute only.
A program may use at most 128 MiB of HBM per device.

```python
import math
import jax
import jax.numpy as jnp
from jax import lax

D = 2048
FF = 512
BR = 1024
GROUPS = 4
TOK_DEV = 768
EXPERTS = 8
CAP = 384
TOKENS = 6144
N_EP = 8
N_TP = 4


def draw_tokens(key, part):
    first, second = jax.random.split(key, 2)
    base = jax.random.normal(first, (TOKENS, D), jnp.float32)
    scales = jnp.exp(jax.random.uniform(second, (N_TP,), jnp.float32, math.log(0.3), math.log(3.0)))
    values = base.reshape(TOKENS, N_TP, D // N_TP) * scales[None, :, None]
    return values.reshape(TOKENS, D).astype(jnp.bfloat16)


def draw_routing(key, part):
    per_group = EXPERTS // GROUPS
    half = TOK_DEV // 2

    def one_block(block):
        block_key = jax.random.fold_in(key, block)
        keys = jax.random.split(block_key, 3 + GROUPS)
        busiest = jax.random.randint(keys[0], (), 0, GROUPS)
        cuts = jax.random.randint(keys[1], (2,), 0, half + 1)
        lower = jnp.min(cuts)
        upper = jnp.max(cuts)
        others = jnp.stack([lower, upper - lower, half - upper])
        group_ids = jnp.arange(GROUPS, dtype=jnp.int32)
        other_place = jnp.clip(group_ids - (group_ids > busiest).astype(jnp.int32), 0, 2)
        counts = jnp.where(group_ids == busiest, half, others[other_place])
        ends = jnp.cumsum(counts)
        starts = ends - counts
        position = jnp.arange(TOK_DEV, dtype=jnp.int32)
        group = jnp.sum((position[:, None] >= ends[None, :]).astype(jnp.int32), axis=1)
        local = position - starts[group]
        orders = jnp.stack([jax.random.permutation(keys[3 + g], per_group) for g in range(GROUPS)]).astype(jnp.int32)
        offset = 1 + local // per_group % (per_group - 1)
        first = orders[group, local % per_group]
        second = orders[group, (local + offset) % per_group]
        paired = jnp.stack([group * per_group + first, group * per_group + second], axis=1)
        shuffle = jax.random.permutation(keys[2], TOK_DEV)
        return paired[shuffle]
    blocks = jax.vmap(one_block)(jnp.arange(N_EP, dtype=jnp.int32))
    return blocks.reshape(TOKENS, 2).astype(jnp.int32)


def levels(rng, shape, cuts, low, high):
    def one(dim, shards_of):
        heights = jax.random.uniform(jax.random.fold_in(jax.random.fold_in(rng, 6), dim), (shards_of,), jnp.float32, low / len(cuts), high / len(cuts))
        return jnp.repeat(jnp.exp(heights), shape[dim] // shards_of).reshape((-1,) + (1,) * (len(shape) - dim - 1))

    gain = one(*cuts[0])
    for cut in cuts[1:]:
        gain = gain * one(*cut)
    return gain


def normal_values(own_key, extent, spread, most, cuts=(), held_as=jnp.bfloat16):
    level = levels(own_key, extent, cuts, -0.22, 0.18) if cuts else 1.0
    array = jax.random.normal(own_key, extent, jnp.float32) * spread * level
    return jnp.minimum(jnp.maximum(array, -most), most).astype(held_as)


def setup_inputs(seed: int = 0) -> dict:
    splits = jax.random.split(jax.random.key(seed), 11)
    return {
        "tokens": draw_tokens(jax.random.fold_in(splits[10], 71), 0),
        "norm_gain": jnp.clip(1.0 + 0.18 * jax.random.normal(splits[1], (D,), jnp.float32), 0.1, 1.9),
        "routing": draw_routing(jax.random.fold_in(splits[10], 71), 0),
        "route_weight": jnp.clip(0.2 + 0.8 * jax.random.uniform(splits[3], (TOKENS, 2), jnp.float32) ** levels(splits[3], (TOKENS, 2), ((0, 8),), -0.2, 0.2), 0.2, 1.0),
        "w_gate": normal_values(splits[4], (EXPERTS, D, FF), D ** -0.5, 0.125, ((0, 8), (1, 4))),
        "w_up": normal_values(splits[5], (EXPERTS, D, FF), D ** -0.5, 0.125, ((0, 8), (1, 4))),
        "w_down": normal_values(splits[6], (EXPERTS, FF, D), FF ** -0.5, 0.25, ((0, 8), (2, 4))),
        "w_branch_in": normal_values(splits[7], (D, BR), D ** -0.5, 0.125, ((0, 8), (1, 4))),
        "w_branch_out": normal_values(splits[8], (BR, D), BR ** -0.5, 0.1875, ((0, 4), (1, 8))),
        "branch_gate": jnp.clip(jax.random.uniform(splits[9], (D,), jnp.float32, -3.0, 3.0) * levels(splits[9], (D,), ((0, 4),), -0.4, 0.0), -3.0, 3.0),
    }


epsilon = 1e-06

def slot_numbers(routing):
    flat_ids = routing.reshape(N_EP, TOK_DEV * 2)
    one_hot = (flat_ids[:, :, None] == jnp.arange(EXPERTS, dtype=jnp.int32)[None, None, :]).astype(jnp.int32)
    before = jnp.cumsum(one_hot, axis=1) - one_hot
    return lax.optimization_barrier(jnp.sum(before * one_hot, axis=2)).reshape(TOKENS, 2).astype(jnp.int32)

def expert(operands):
    inputs, gate_weight, up_weight, down_weight = operands
    gate_sum = jnp.dot(inputs, gate_weight, preferred_element_type=jnp.float32)
    up_sum = jnp.dot(inputs, up_weight, preferred_element_type=jnp.float32)
    hidden = (jax.nn.silu(gate_sum) * up_sum).astype(jnp.bfloat16)
    return jnp.dot(hidden, down_weight, preferred_element_type=jnp.float32).astype(jnp.bfloat16)

def reference(tokens, norm_gain, routing, route_weight, w_gate, w_up, w_down, w_branch_in, w_branch_out, branch_gate):
    floats = tokens.astype(jnp.float32)
    squares = lax.optimization_barrier(jnp.mean(floats * floats, axis=1, keepdims=True))
    normed = (floats * lax.rsqrt(squares + epsilon) * norm_gain).astype(jnp.bfloat16)
    source = (jnp.arange(TOKENS, dtype=jnp.int32) // TOK_DEV)[:, None]
    place = (source * CAP + slot_numbers(routing)).astype(jnp.int32)
    copies = jnp.broadcast_to(normed[:, None, :], (TOKENS, 2, D))
    buffer = jnp.zeros((EXPERTS, N_EP * CAP, D), jnp.bfloat16).at[routing, place].set(copies)
    outputs = lax.map(expert, (buffer, w_gate, w_up, w_down))
    picked = outputs[routing, place].astype(jnp.float32)
    routed = lax.optimization_barrier(jnp.sum(picked * route_weight[:, :, None], axis=1))
    branch_hidden = jax.nn.silu(jnp.dot(normed, w_branch_in, preferred_element_type=jnp.float32)).astype(jnp.bfloat16)
    branch = jnp.dot(branch_hidden, w_branch_out, preferred_element_type=jnp.float32).astype(jnp.bfloat16)
    return (routed + jax.nn.sigmoid(branch_gate) * branch.astype(jnp.float32)).astype(jnp.bfloat16)
```

```python
import jax
import jax.numpy as jnp
from jax import lax
from jax.sharding import Mesh, PartitionSpec as P

GROUPS = 4

epsilon = 1e-06


def flip(value, axis, bit):
    size = lax.axis_size(axis)
    return lax.ppermute(value, axis, [(i, i ^ bit) for i in range(size)])


def normalize(rows, gain):
    floats = rows.astype(jnp.float32)
    squares = jnp.mean(floats * floats, axis=1, keepdims=True)
    return (floats * lax.rsqrt(squares + epsilon) * gain).astype(jnp.bfloat16)


def dot(a, b):
    return jnp.dot(a, b, preferred_element_type=jnp.float32)


def pair_body(
    tokens,
    norm_gain,
    routing,
    route_weight,
    w_gate,
    w_up,
    w_down,
    w_branch_in,
    w_branch_out,
    branch_gate,
):
    token_count, quarter = tokens.shape
    groups = lax.axis_size("grp")
    parts = lax.axis_size("tp")
    members = lax.axis_size("mem")
    capacity = token_count // 2
    share = capacity // parts
    me = lax.axis_index("tp")
    slots = groups * capacity

    group = routing[:, 0] // members
    one_hot = (group[:, None] == jnp.arange(groups, dtype=jnp.int32)[None, :]).astype(jnp.bfloat16)
    row = lax.broadcasted_iota(jnp.int32, (token_count, token_count), 0)
    col = lax.broadcasted_iota(jnp.int32, (token_count, token_count), 1)
    before = dot((row > col).astype(jnp.bfloat16), one_hot)
    rank = jnp.sum(before * one_hot.astype(jnp.float32), axis=1).astype(jnp.int32)
    slot = group * capacity + rank
    place = jnp.arange(slots, dtype=jnp.int32)[:, None] == slot[None, :]
    buffer = dot(place.astype(jnp.bfloat16), tokens).astype(jnp.bfloat16)
    member = routing % members
    weight = jnp.stack(
        [jnp.sum(jnp.where(member == j, route_weight, 0.0), axis=1) for j in range(2)], axis=0
    )
    slot_weight = jnp.dot(
        weight, place.T.astype(jnp.float32), precision=lax.Precision.HIGHEST
    )

    meta = jnp.concatenate(
        [
            slot_weight.reshape(2, groups * parts, share).transpose(1, 0, 2).reshape(groups * parts, 2 * share),
            jnp.broadcast_to(norm_gain[None, :], (groups * parts, quarter)),
        ],
        axis=1,
    )
    meta = lax.all_to_all(meta[:, None, :], ("grp", "tp"), 0, 0, tiled=True).reshape(
        groups, parts, 2 * share + quarter
    )
    gain = meta[0, :, 2 * share :].reshape(1, parts * quarter)
    own_weight = meta[:, 0, : 2 * share].reshape(groups, 2, share)
    arrived = lax.all_to_all(
        buffer.reshape(groups * parts, share, quarter), ("grp", "tp"), 0, 0, tiled=True
    ).reshape(groups, parts, share, quarter)

    own = [w_gate[0], w_up[0], w_down[0]]
    across = [flip(w, "tp", 2) for w in own]
    other = [flip(w, "mem", 1) for w in own]
    diagonal = [
        flip(across[0], "mem", 1),
        flip(across[1], "mem", 1),
        flip(other[2], "tp", 2),
    ]
    sets = []
    for near, far in ((own, across), (other, diagonal)):
        near_pair = [flip(w, "tp", 1) for w in near]
        far_pair = [flip(w, "tp", 1) for w in far]
        sets.append([near, near_pair, far, far_pair])

    order = [me ^ k for k in range(parts)]
    features = arrived.transpose(1, 0, 2, 3).reshape(parts, groups * share, quarter)
    whole = features.transpose(1, 0, 2).reshape(groups * share, parts * quarter)
    normed = normalize(whole, gain).reshape(groups * share, parts, quarter)
    pieces = [lax.dynamic_index_in_dim(normed, q, axis=1, keepdims=False) for q in order]
    side = lax.axis_index("mem")
    first = jnp.where(side == 0, own_weight[:, 0], own_weight[:, 1]).reshape(-1, 1)
    second = jnp.where(side == 0, own_weight[:, 1], own_weight[:, 0]).reshape(-1, 1)
    hiddens = []
    for weights in sets:
        gate_sum = sum(dot(pieces[k], weights[k][0]) for k in range(parts))
        up_sum = sum(dot(pieces[k], weights[k][1]) for k in range(parts))
        hiddens.append((jax.nn.silu(gate_sum) * up_sum).astype(jnp.bfloat16))
    results = jnp.zeros((parts, groups, share, quarter), jnp.bfloat16)
    for k in range(parts):
        left = dot(hiddens[0], sets[0][k][2]).astype(jnp.bfloat16).astype(jnp.float32)
        right = dot(hiddens[1], sets[1][k][2]).astype(jnp.bfloat16).astype(jnp.float32)
        mix = (first * left + second * right).astype(jnp.bfloat16)
        results = lax.dynamic_update_index_in_dim(
            results, mix.reshape(groups, share, quarter), order[k], axis=0
        )
    returned = lax.all_to_all(
        results.transpose(1, 0, 2, 3).reshape(groups * parts, share, quarter),
        ("grp", "tp"),
        0,
        0,
        tiled=True,
    ).reshape(slots, quarter)
    routed = dot(place.astype(jnp.bfloat16).T, returned)

    far_tokens = flip(tokens, "tp", 2)
    token_parts = [tokens, flip(tokens, "tp", 1), far_tokens, flip(far_tokens, "tp", 1)]
    branch_weights = jnp.stack([w_branch_in, w_branch_out], axis=0)
    spread = lax.all_to_all(
        jnp.broadcast_to(branch_weights[None], (groups,) + branch_weights.shape),
        "grp",
        0,
        0,
        tiled=True,
    )
    spread_other = flip(spread, "mem", 1)
    low = jnp.where(side == 0, spread, spread_other)
    high = jnp.where(side == 0, spread_other, spread)
    in_parts = jnp.concatenate([low[:, 0], high[:, 0]], axis=1)
    out_parts = jnp.concatenate([low[:, 1], high[:, 1]], axis=2)
    squares = sum(
        jnp.sum(t.astype(jnp.float32) * t.astype(jnp.float32), axis=1, keepdims=True)
        for t in token_parts
    ) / (parts * quarter)
    scale = lax.rsqrt(squares + epsilon)
    gains = gain.reshape(parts, quarter)
    hidden_sum = 0.0
    for k in range(parts):
        own_gain = lax.dynamic_index_in_dim(gains, order[k], axis=0, keepdims=True)
        own_rows = lax.dynamic_index_in_dim(in_parts, order[k], axis=0, keepdims=False)
        normed_part = (token_parts[k].astype(jnp.float32) * scale * own_gain[0]).astype(jnp.bfloat16)
        hidden_sum = hidden_sum + dot(normed_part, own_rows)
    branch_hidden = jax.nn.silu(hidden_sum).astype(jnp.bfloat16)
    partial = [
        dot(branch_hidden, lax.dynamic_index_in_dim(out_parts, q, axis=0, keepdims=False))
        for q in order
    ]
    near = partial[0] + flip(partial[1].astype(jnp.bfloat16), "tp", 1).astype(jnp.float32)
    far = partial[2] + flip(partial[3].astype(jnp.bfloat16), "tp", 1).astype(jnp.float32)
    branch = near + flip(far.astype(jnp.bfloat16), "tp", 2).astype(jnp.float32)
    branch = branch.astype(jnp.bfloat16).astype(jnp.float32)
    return (routed + jax.nn.sigmoid(branch_gate) * branch).astype(jnp.bfloat16)


def send_back(result):
    return lax.all_to_all(result, "ep", split_axis=0, concat_axis=0, tiled=True)


def body(
    tokens,
    norm_gain,
    routing,
    route_weight,
    w_gate,
    w_up,
    w_down,
    w_branch_in,
    w_branch_out,
    branch_gate,
):
    token_count, quarter = tokens.shape
    full_width = quarter * lax.axis_size("tp")
    floats = tokens.astype(jnp.float32)
    squares = lax.psum(jnp.sum(floats * floats, axis=1), "tp")
    normed = (floats * lax.rsqrt(squares[:, None] / full_width + epsilon) * norm_gain).astype(
        jnp.bfloat16
    )
    expert_count = lax.axis_size("ep") * w_gate.shape[0]
    capacity = token_count // (expert_count // GROUPS)
    flat_ids = routing.reshape(-1)
    one_hot = (flat_ids[:, None] == jnp.arange(expert_count, dtype=jnp.int32)[None, :]).astype(
        jnp.int32
    )
    before = jnp.cumsum(one_hot, axis=0) - one_hot
    position = flat_ids * capacity + jnp.sum(before * one_hot, axis=1)
    copies = jnp.repeat(normed, 2, axis=0)
    buffer = jnp.zeros((expert_count * capacity, quarter), jnp.bfloat16).at[position].set(copies)
    buffer = buffer.reshape(expert_count, capacity, quarter)
    gate_whole, up_whole, down_whole = (
        lax.all_gather(w_gate[0], "tp", axis=0, tiled=True),
        lax.all_gather(w_up[0], "tp", axis=0, tiled=True),
        lax.all_gather(w_down[0], "tp", axis=1, tiled=True),
    )
    row_split = lax.all_to_all(
        lax.all_to_all(buffer, "ep", split_axis=0, concat_axis=0, tiled=True),
        "tp",
        split_axis=0,
        concat_axis=2,
        tiled=True,
    )
    slot_rows = row_split.reshape(-1, row_split.shape[2])
    gate_sum = jnp.dot(slot_rows, gate_whole, preferred_element_type=jnp.float32)
    up_sum = jnp.dot(slot_rows, up_whole, preferred_element_type=jnp.float32)
    hidden = (jax.nn.silu(gate_sum) * up_sum).astype(jnp.bfloat16)
    result = jnp.dot(hidden, down_whole, preferred_element_type=jnp.float32).astype(jnp.bfloat16)
    feature_split = lax.all_to_all(
        result.reshape(row_split.shape), "tp", split_axis=2, concat_axis=0, tiled=True
    )
    returned = send_back(feature_split)
    picked = returned.reshape(expert_count * capacity, quarter)[position].reshape(
        token_count, 2, quarter
    )
    routed = jnp.sum(picked.astype(jnp.float32) * route_weight[:, :, None], axis=1)
    branch_tokens = lax.all_to_all(normed, "tp", split_axis=0, concat_axis=1, tiled=True)
    in_cols, out_rows = (
        lax.all_gather(w_branch_in, "tp", axis=1, tiled=True),
        lax.all_gather(w_branch_out, "tp", axis=0, tiled=True),
    )
    in_whole, out_whole = (
        lax.all_gather(in_cols, "ep", axis=0, tiled=True),
        lax.all_gather(out_rows, "ep", axis=1, tiled=True),
    )
    branch_hidden = jax.nn.silu(
        jnp.dot(branch_tokens, in_whole, preferred_element_type=jnp.float32)
    ).astype(jnp.bfloat16)
    branch_local = jnp.dot(branch_hidden, out_whole, preferred_element_type=jnp.float32).astype(
        jnp.bfloat16
    )
    branch = lax.all_to_all(branch_local, "tp", split_axis=1, concat_axis=0, tiled=True)
    return (routed + jax.nn.sigmoid(branch_gate) * branch.astype(jnp.float32)).astype(jnp.bfloat16)


def solution(mesh):
    shape = dict(mesh.shape)
    members = shape["ep"] // GROUPS
    if members == 2 and shape["tp"] == 4:
        ep = ("grp", "mem")
        mesh = Mesh(
            mesh.devices.reshape(GROUPS, members, shape["tp"]), ("grp", "mem", "tp")
        )
        part = pair_body
    else:
        ep = "ep"
        part = body
    return jax.shard_map(
        part,
        mesh=mesh,
        in_specs=(
            P(ep, "tp"),
            P("tp"),
            P(ep, None),
            P(ep, None),
            P(ep, "tp", None),
            P(ep, "tp", None),
            P(ep, None, "tp"),
            P(ep, "tp"),
            P("tp", ep),
            P("tp"),
        ),
        out_specs=P(ep, "tp"),
        check_vma=False,
    )
```

```python
import functools

import jax
import jax.numpy as jnp
from jax import lax
from jax.experimental import pallas as pl
from jax.experimental.pallas import tpu as pltpu
from jax.sharding import Mesh, PartitionSpec as P


GROUPS = 4

epsilon = 1e-06


def flip(value, axis, bit):
    size = lax.axis_size(axis)
    return lax.ppermute(value, axis, [(i, i ^ bit) for i in range(size)])


def dot(a, b):
    return jnp.dot(a, b, preferred_element_type=jnp.float32)


def slots_kernel(ids_ref, weight_ref, token_ref, buffer_ref, slot_ref, *, groups, members, parts):
    tokens = token_ref.shape[0]
    capacity = tokens // 2
    share = capacity // parts
    ids = ids_ref[...]
    weights = weight_ref[...]
    rows = lax.broadcasted_iota(jnp.int32, (8, tokens), 0)
    low = rows * members
    hot = ((ids[0:1] >= low) & (ids[0:1] < low + members) & (rows < groups)).astype(jnp.float32)
    earlier = lax.broadcasted_iota(jnp.int32, (tokens, tokens), 0) < lax.broadcasted_iota(
        jnp.int32, (tokens, tokens), 1
    )
    before = dot(hot.astype(jnp.bfloat16), earlier.astype(jnp.float32).astype(jnp.bfloat16))
    rank = jnp.sum(before * hot, axis=0, keepdims=True).astype(jnp.int32)
    group = jnp.sum(hot * rows.astype(jnp.float32), axis=0, keepdims=True).astype(jnp.int32)
    slot = group * capacity + rank
    slot_ref[...] = slot
    member = ids - group * members
    terms = jnp.zeros((8, tokens), jnp.float32)
    for j in range(members):
        left = jnp.sum(jnp.where(member == j, weights, 0.0), axis=0, keepdims=True)
        for i in range(3):
            term = left.astype(jnp.bfloat16).astype(jnp.float32)
            terms = jnp.where(rows == 3 * j + i, term, terms)
            left = left - term
    terms = terms.astype(jnp.bfloat16)
    values = token_ref[...]
    index = lax.broadcasted_iota(jnp.int32, (capacity, tokens), 0)
    for g in range(groups):
        place = (index + g * capacity == slot).astype(jnp.float32).astype(jnp.bfloat16)
        moved = dot(place, values).astype(jnp.bfloat16)
        carried = lax.dot_general(
            terms, place, (((1,), (1,)), ((), ())), preferred_element_type=jnp.float32
        ).astype(jnp.bfloat16)
        for q in range(parts):
            block = g * parts + q
            part = slice(q * share, (q + 1) * share)
            buffer_ref[block, :share, :] = moved[part]
            buffer_ref[block, share:, :] = jnp.zeros((8, values.shape[1]), jnp.bfloat16)
            buffer_ref[block, share:, :share] = carried[:, part]


def experts_kernel(where_ref, gain_ref, rows_ref, *refs, parts):
    count = 6 * parts
    weights, out_ref, held, normed, copied = refs[:count], *refs[count:]
    groups = rows_ref.shape[0]
    share = out_ref.shape[2]
    quarter = out_ref.shape[3]
    total = groups * share
    me, side = where_ref[0], where_ref[1]
    copies = [
        pltpu.make_async_copy(weights[i], held.at[i], copied.at[i]) for i in range(count)
    ]
    for copy in copies:
        copy.start()
    squares = jnp.zeros((total, 1), jnp.float32)
    for q in range(parts):
        part = rows_ref[:, q, :share, :].reshape(total, quarter).astype(jnp.float32)
        squares = squares + jnp.sum(part * part, axis=1, keepdims=True)
    scale = lax.rsqrt(squares / (parts * quarter) + epsilon)
    for k in range(parts):
        part = rows_ref[:, me ^ k, :share, :].reshape(total, quarter).astype(jnp.float32)
        normed[k] = (part * scale * gain_ref[k : k + 1, :]).astype(jnp.bfloat16)
    hidden = []
    for e in range(2):
        sums = []
        for m in range(2):
            value = None
            for k in range(parts):
                i = (e * 3 + m) * parts + k
                copies[i].wait()
                term = dot(normed[k], held[i])
                value = term if value is None else value + term
            sums.append(value)
        gate, up = sums
        hidden.append((gate / (1.0 + jnp.exp(-gate)) * up).astype(jnp.bfloat16))
    columns = []
    for g in range(groups):
        block = rows_ref[g, 0, share:, :share].astype(jnp.float32)
        block = jnp.concatenate(
            [block, jnp.zeros((8, 128 - share), jnp.float32)], axis=1
        ).T[:share]
        columns.append(
            [block[:, 3 * j : 3 * j + 1] + block[:, 3 * j + 1 : 3 * j + 2] + block[:, 3 * j + 2 : 3 * j + 3] for j in range(2)]
        )
    by_member = [jnp.concatenate([c[j] for c in columns], axis=0) for j in range(2)]
    first = jnp.where(side == 0, by_member[0], by_member[1])
    second = jnp.where(side == 0, by_member[1], by_member[0])
    for k in range(parts):
        mix = None
        for e, weight in ((0, first), (1, second)):
            i = (e * 3 + 2) * parts + k
            copies[i].wait()
            value = dot(hidden[e], held[i]).astype(jnp.bfloat16).astype(jnp.float32) * weight
            mix = value if mix is None else mix + value
        out_ref[:, me ^ k, :, :] = mix.astype(jnp.bfloat16).reshape(groups, share, quarter)


def finish_kernel(slot_ref, rows_ref, near_ref, far_ref, gate_ref, out_ref):
    tokens = out_ref.shape[0]
    slots = rows_ref.shape[0]
    index = lax.broadcasted_iota(jnp.int32, (tokens, slots), 1)
    place = (index == slot_ref[...]).astype(jnp.float32).astype(jnp.bfloat16)
    routed = dot(place, rows_ref[...])
    branch = (near_ref[...] + far_ref[...].astype(jnp.float32)).astype(jnp.bfloat16)
    gate = 1.0 / (1.0 + jnp.exp(-gate_ref[...]))
    out_ref[...] = (routed + gate * branch.astype(jnp.float32)).astype(jnp.bfloat16)


VMEM = pl.BlockSpec(memory_space=pltpu.VMEM)
SMEM = pl.BlockSpec(memory_space=pltpu.SMEM)
ANY = pl.BlockSpec(memory_space=pl.ANY)


def pair_body(*arguments):
    return pair_layer(*arguments)


def pair_layer(
    tokens,
    norm_gain,
    routing,
    route_weight,
    w_gate,
    w_up,
    w_down,
    w_branch_in,
    w_branch_out,
    branch_gate,
):
    token_count, quarter = tokens.shape
    groups = lax.axis_size("grp")
    parts = lax.axis_size("tp")
    members = lax.axis_size("mem")
    capacity = token_count // 2
    share = capacity // parts
    me = lax.axis_index("tp")
    side = lax.axis_index("mem")
    slots = groups * capacity

    own = [w_gate[0], w_up[0], w_down[0]]
    across, other, diagonal = [], [], []
    for w in own:
        across.append(flip(w, "tp", 2))
        other.append(flip(w, "mem", 1))
    for w in across:
        diagonal.append(flip(w, "mem", 1))
    sets = []
    for near, far in ((own, across), (other, diagonal)):
        near_pair = [flip(w, "tp", 1) for w in near]
        far_pair = [flip(w, "tp", 1) for w in far]
        sets.append([near, near_pair, far, far_pair])

    gain = norm_gain[None, :]
    far_gain = flip(gain, "tp", 2)
    gains = jnp.concatenate([gain, flip(gain, "tp", 1), far_gain, flip(far_gain, "tp", 1)], axis=0)

    buffer, slot = pl.pallas_call(
        functools.partial(slots_kernel, groups=groups, members=members, parts=parts),
        out_shape=(
            jax.ShapeDtypeStruct((groups * parts, share + 8, quarter), jnp.bfloat16),
            jax.ShapeDtypeStruct((1, token_count), jnp.int32),
        ),
        in_specs=[VMEM] * 3,
        out_specs=(VMEM, VMEM),
        name="slots",
    )(routing.T, route_weight.T, tokens)
    arrived = lax.all_to_all(buffer, ("grp", "tp"), 0, 0, tiled=True)
    arrived = arrived.reshape(groups, parts, share + 8, quarter)

    flat = [sets[e][k][m] for e in range(2) for m in range(3) for k in range(parts)]
    results = pl.pallas_call(
        functools.partial(experts_kernel, parts=parts),
        out_shape=jax.ShapeDtypeStruct((groups, parts, share, quarter), jnp.bfloat16),
        in_specs=[SMEM, VMEM, VMEM] + [ANY] * len(flat),
        out_specs=VMEM,
        scratch_shapes=[
            pltpu.VMEM((len(flat),) + flat[0].shape, jnp.bfloat16),
            pltpu.VMEM((parts, groups * share, quarter), jnp.bfloat16),
            pltpu.SemaphoreType.DMA((len(flat),)),
        ],
        name="experts",
    )(jnp.stack([me, side]), gains, arrived, *flat)
    returned = lax.all_to_all(
        results.reshape(groups * parts, share, quarter), ("grp", "tp"), 0, 0, tiled=True
    )

    far_tokens = flip(tokens, "tp", 2)
    token_parts = [tokens, flip(tokens, "tp", 1), far_tokens, flip(far_tokens, "tp", 1)]
    own_pair = jnp.stack([w_branch_in, w_branch_out], axis=0)
    level = lax.axis_index("grp")
    spread = [own_pair]
    for k in range(1, groups):
        spread.append(flip(own_pair, "grp", k))
    spread = jnp.stack(spread, axis=0)
    spread_other = flip(spread, "mem", 1)
    low = jnp.where(side == 0, spread, spread_other)
    high = jnp.where(side == 0, spread_other, spread)
    in_parts = jnp.concatenate([low[:, 0], high[:, 0]], axis=1)
    out_parts = jnp.concatenate([low[:, 1], high[:, 1]], axis=2)
    squares = sum(
        jnp.sum(t.astype(jnp.float32) * t.astype(jnp.float32), axis=1, keepdims=True)
        for t in token_parts
    ) / (parts * quarter)
    scale = lax.rsqrt(squares + epsilon)
    hidden_sum = 0.0
    for k in range(parts):
        own_rows = lax.dynamic_index_in_dim(in_parts, level ^ me ^ k, axis=0, keepdims=False)
        normed_part = (token_parts[k].astype(jnp.float32) * scale * gains[k]).astype(jnp.bfloat16)
        hidden_sum = hidden_sum + dot(normed_part, own_rows)
    branch_hidden = jax.nn.silu(hidden_sum).astype(jnp.bfloat16)
    partial = [
        dot(
            branch_hidden,
            lax.dynamic_index_in_dim(out_parts, level ^ me ^ k, axis=0, keepdims=False),
        )
        for k in range(parts)
    ]
    far = partial[2] + flip(partial[3].astype(jnp.bfloat16), "tp", 1).astype(jnp.float32)
    far = flip(far.astype(jnp.bfloat16), "tp", 2)
    near = partial[0] + flip(partial[1].astype(jnp.bfloat16), "tp", 1).astype(jnp.float32)
    return pl.pallas_call(
        finish_kernel,
        out_shape=jax.ShapeDtypeStruct((token_count, quarter), jnp.bfloat16),
        in_specs=[VMEM] * 5,
        out_specs=VMEM,
        name="finish",
    )(
        slot.reshape(token_count, 1),
        returned.reshape(slots, quarter),
        near,
        far,
        branch_gate[None, :],
    )


def send_back(result):
    return lax.all_to_all(result, "ep", split_axis=0, concat_axis=0, tiled=True)


def body(
    tokens,
    norm_gain,
    routing,
    route_weight,
    w_gate,
    w_up,
    w_down,
    w_branch_in,
    w_branch_out,
    branch_gate,
):
    token_count, quarter = tokens.shape
    full_width = quarter * lax.axis_size("tp")
    floats = tokens.astype(jnp.float32)
    squares = lax.psum(jnp.sum(floats * floats, axis=1), "tp")
    normed = (floats * lax.rsqrt(squares[:, None] / full_width + epsilon) * norm_gain).astype(
        jnp.bfloat16
    )
    expert_count = lax.axis_size("ep") * w_gate.shape[0]
    capacity = token_count // (expert_count // GROUPS)
    flat_ids = routing.reshape(-1)
    one_hot = (flat_ids[:, None] == jnp.arange(expert_count, dtype=jnp.int32)[None, :]).astype(
        jnp.int32
    )
    before = jnp.cumsum(one_hot, axis=0) - one_hot
    position = flat_ids * capacity + jnp.sum(before * one_hot, axis=1)
    copies = jnp.repeat(normed, 2, axis=0)
    buffer = jnp.zeros((expert_count * capacity, quarter), jnp.bfloat16).at[position].set(copies)
    buffer = buffer.reshape(expert_count, capacity, quarter)
    gate_whole, up_whole, down_whole = (
        lax.all_gather(w_gate[0], "tp", axis=0, tiled=True),
        lax.all_gather(w_up[0], "tp", axis=0, tiled=True),
        lax.all_gather(w_down[0], "tp", axis=1, tiled=True),
    )
    row_split = lax.all_to_all(
        lax.all_to_all(buffer, "ep", split_axis=0, concat_axis=0, tiled=True),
        "tp",
        split_axis=0,
        concat_axis=2,
        tiled=True,
    )
    slot_rows = row_split.reshape(-1, row_split.shape[2])
    gate_sum = jnp.dot(slot_rows, gate_whole, preferred_element_type=jnp.float32)
    up_sum = jnp.dot(slot_rows, up_whole, preferred_element_type=jnp.float32)
    hidden = (jax.nn.silu(gate_sum) * up_sum).astype(jnp.bfloat16)
    result = jnp.dot(hidden, down_whole, preferred_element_type=jnp.float32).astype(jnp.bfloat16)
    feature_split = lax.all_to_all(
        result.reshape(row_split.shape), "tp", split_axis=2, concat_axis=0, tiled=True
    )
    returned = send_back(feature_split)
    picked = returned.reshape(expert_count * capacity, quarter)[position].reshape(
        token_count, 2, quarter
    )
    routed = jnp.sum(picked.astype(jnp.float32) * route_weight[:, :, None], axis=1)
    branch_tokens = lax.all_to_all(normed, "tp", split_axis=0, concat_axis=1, tiled=True)
    in_cols, out_rows = (
        lax.all_gather(w_branch_in, "tp", axis=1, tiled=True),
        lax.all_gather(w_branch_out, "tp", axis=0, tiled=True),
    )
    in_whole, out_whole = (
        lax.all_gather(in_cols, "ep", axis=0, tiled=True),
        lax.all_gather(out_rows, "ep", axis=1, tiled=True),
    )
    branch_hidden = jax.nn.silu(
        jnp.dot(branch_tokens, in_whole, preferred_element_type=jnp.float32)
    ).astype(jnp.bfloat16)
    branch_local = jnp.dot(branch_hidden, out_whole, preferred_element_type=jnp.float32).astype(
        jnp.bfloat16
    )
    branch = lax.all_to_all(branch_local, "tp", split_axis=1, concat_axis=0, tiled=True)
    return (routed + jax.nn.sigmoid(branch_gate) * branch.astype(jnp.float32)).astype(jnp.bfloat16)


def solution(mesh):
    shape = dict(mesh.shape)
    members = shape["ep"] // GROUPS
    paired = members == 2 and shape["tp"] == 4
    if paired:
        ep = ("grp", "mem")
        mesh = Mesh(
            mesh.devices.reshape(GROUPS, members, shape["tp"]), ("grp", "mem", "tp")
        )
    else:
        ep = "ep"
    return jax.shard_map(
        pair_body if paired else body,
        mesh=mesh,
        in_specs=(
            P(ep, "tp"),
            P("tp"),
            P(ep, None),
            P(ep, None),
            P(ep, "tp", None),
            P(ep, "tp", None),
            P(ep, None, "tp"),
            P(ep, "tp"),
            P("tp", ep),
            P("tp"),
        ),
        out_specs=P(ep, "tp"),
        check_vma=False,
    )
```

```python
import functools

import jax
import jax.numpy as jnp
from jax import lax
from jax.experimental import pallas as pl
from jax.experimental.pallas import tpu as pltpu
from jax.sharding import Mesh, PartitionSpec as P


GROUPS = 4

epsilon = 1e-06


def flip(value, axis, bit):
    size = lax.axis_size(axis)
    return lax.ppermute(value, axis, [(i, i ^ bit) for i in range(size)])


def dot(a, b):
    return jnp.dot(a, b, preferred_element_type=jnp.float32)


def slots_kernel(ids_ref, weight_ref, token_ref, buffer_ref, slot_ref, *, groups, members, parts):
    tokens = token_ref.shape[0]
    capacity = tokens // 2
    share = capacity // parts
    ids = ids_ref[...]
    weights = weight_ref[...]
    rows = lax.broadcasted_iota(jnp.int32, (8, tokens), 0)
    low = rows * members
    hot = ((ids[0:1] >= low) & (ids[0:1] < low + members) & (rows < groups)).astype(jnp.float32)
    earlier = lax.broadcasted_iota(jnp.int32, (tokens, tokens), 0) < lax.broadcasted_iota(
        jnp.int32, (tokens, tokens), 1
    )
    before = dot(hot.astype(jnp.bfloat16), earlier.astype(jnp.float32).astype(jnp.bfloat16))
    rank = jnp.sum(before * hot, axis=0, keepdims=True).astype(jnp.int32)
    group = jnp.sum(hot * rows.astype(jnp.float32), axis=0, keepdims=True).astype(jnp.int32)
    slot = group * capacity + rank
    slot_ref[...] = slot
    member = ids - group * members
    terms = jnp.zeros((8, tokens), jnp.float32)
    for j in range(members):
        left = jnp.sum(jnp.where(member == j, weights, 0.0), axis=0, keepdims=True)
        for i in range(3):
            term = left.astype(jnp.bfloat16).astype(jnp.float32)
            terms = jnp.where(rows == 3 * j + i, term, terms)
            left = left - term
    terms = terms.astype(jnp.bfloat16)
    values = token_ref[...]
    index = lax.broadcasted_iota(jnp.int32, (capacity, tokens), 0)
    for g in range(groups):
        place = (index + g * capacity == slot).astype(jnp.float32).astype(jnp.bfloat16)
        moved = dot(place, values).astype(jnp.bfloat16)
        carried = lax.dot_general(
            terms, place, (((1,), (1,)), ((), ())), preferred_element_type=jnp.float32
        ).astype(jnp.bfloat16)
        for q in range(parts):
            block = g * parts + q
            part = slice(q * share, (q + 1) * share)
            buffer_ref[block, :share, :] = moved[part]
            buffer_ref[block, share:, :] = jnp.zeros((8, values.shape[1]), jnp.bfloat16)
            buffer_ref[block, share:, :share] = carried[:, part]


def rows_kernel(gain0, gain1, gain2, gain3, rows_ref, normed_ref, weight_ref):
    gains = (gain0, gain1, gain2, gain3)
    parts, total, quarter = normed_ref.shape
    groups = rows_ref.shape[0]
    share = total // groups
    me = lax.axis_index("tp")
    side = lax.axis_index("mem")
    squares = jnp.zeros((total, 1), jnp.float32)
    for q in range(parts):
        part = rows_ref[:, q, :share, :].reshape(total, quarter).astype(jnp.float32)
        squares = squares + jnp.sum(part * part, axis=1, keepdims=True)
    scale = lax.rsqrt(squares / (parts * quarter) + epsilon)
    for k in range(parts):
        part = rows_ref[:, me ^ k, :share, :].reshape(total, quarter).astype(jnp.float32)
        normed_ref[k] = (part * scale * gains[k][...]).astype(jnp.bfloat16)
    columns = []
    for g in range(groups):
        block = rows_ref[g, 0, share:, :128].astype(jnp.float32).T[:share]
        columns.append(
            [sum(block[:, 3 * j + i : 3 * j + i + 1] for i in range(3)) for j in range(2)]
        )
    by_member = [jnp.concatenate([c[j] for c in columns], axis=0) for j in range(2)]
    weight_ref[0] = jnp.where(side == 0, by_member[0], by_member[1])
    weight_ref[1] = jnp.where(side == 0, by_member[1], by_member[0])


def hidden_kernel(normed_ref, *refs):
    parts, _, _ = normed_ref.shape
    count = 4 * parts
    weights, out_ref, held, copied = refs[:count], *refs[count:]
    copies = [
        pltpu.make_async_copy(weights[i], held.at[i], copied.at[i]) for i in range(count)
    ]
    for copy in copies:
        copy.start()
    for e in range(2):
        sums = []
        for m in range(2):
            value = None
            for k in range(parts):
                i = (e * 2 + m) * parts + k
                copies[i].wait()
                term = dot(normed_ref[k], held[i])
                value = term if value is None else value + term
            sums.append(value)
        gate, up = sums
        out_ref[e] = (gate / (1.0 + jnp.exp(-gate)) * up).astype(jnp.bfloat16)


def down_kernel(hidden_ref, weight_ref, *refs):
    out_ref, held, copied = refs[-3:]
    groups, parts, share, quarter = out_ref.shape
    count = 2 * parts
    weights = refs[:count]
    me = lax.axis_index("tp")
    copies = [
        pltpu.make_async_copy(weights[i], held.at[i], copied.at[i]) for i in range(count)
    ]
    for copy in copies:
        copy.start()
    for k in range(parts):
        mix = None
        for e in range(2):
            i = 2 * k + e
            copies[i].wait()
            value = dot(hidden_ref[e], held[i]).astype(jnp.bfloat16).astype(jnp.float32)
            value = value * weight_ref[e]
            mix = value if mix is None else mix + value
        out_ref[:, me ^ k, :, :] = mix.astype(jnp.bfloat16).reshape(groups, share, quarter)


def branch_kernel(*refs):
    parts = 4
    gains, tokens, pieces = refs[:parts], refs[parts : 2 * parts], refs[2 * parts : -7]
    own0, send1, own2, send3, in_held, out_held, copied = refs[-7:]
    groups = in_held.shape[0]
    me = lax.axis_index("tp")
    side = lax.axis_index("mem")
    level = lax.axis_index("grp")
    rows, quarter = tokens[0].shape
    depth = in_held.shape[3]
    copies = []
    for n, held in enumerate((in_held, out_held)):
        for o in range(2):
            for j in range(groups):
                i = (2 * n + o) * groups + j
                copy = pltpu.make_async_copy(pieces[i], held.at[j, side ^ o], copied.at[i])
                copy.start()
                copies.append(copy)
    squares = jnp.zeros((rows, 1), jnp.float32)
    for k in range(parts):
        part = tokens[k][...].astype(jnp.float32)
        squares = squares + jnp.sum(part * part, axis=1, keepdims=True)
    scale = lax.rsqrt(squares / (parts * quarter) + epsilon)
    for copy in copies:
        copy.wait()
    value = None
    for k in range(parts):
        part = tokens[k][...].astype(jnp.float32)
        normed = (part * scale * gains[k][...]).astype(jnp.bfloat16)
        term = dot(normed, in_held[level ^ me ^ k].reshape(quarter, depth))
        value = term if value is None else value + term
    hidden = (value / (1.0 + jnp.exp(-value))).astype(jnp.bfloat16)
    for k, ref in enumerate((own0, send1, own2, send3)):
        for y in range(2):
            piece = dot(hidden, out_held[level ^ me ^ k, y])
            width = piece.shape[1]
            ref[:, y * width : (y + 1) * width] = piece.astype(ref.dtype)


def finish_kernel(slot_ref, rows_ref, own_ref, near_ref, far_ref, gate_ref, out_ref):
    tokens = out_ref.shape[0]
    slots = rows_ref.shape[0]
    index = lax.broadcasted_iota(jnp.int32, (tokens, slots), 1)
    place = (index == slot_ref[...]).astype(jnp.float32).astype(jnp.bfloat16)
    routed = dot(place, rows_ref[...])
    branch = own_ref[...] + near_ref[...].astype(jnp.float32) + far_ref[...].astype(jnp.float32)
    gate = 1.0 / (1.0 + jnp.exp(-gate_ref[...]))
    branch = branch.astype(jnp.bfloat16).astype(jnp.float32)
    out_ref[...] = (routed + gate * branch).astype(jnp.bfloat16)


VMEM = pl.BlockSpec(memory_space=pltpu.VMEM)
SMEM = pl.BlockSpec(memory_space=pltpu.SMEM)
ANY = pl.BlockSpec(memory_space=pl.ANY)


def pair_body(*arguments):
    return pair_layer(*arguments)


def pair_layer(
    tokens,
    norm_gain,
    routing,
    route_weight,
    w_gate,
    w_up,
    w_down,
    w_branch_in,
    w_branch_out,
    branch_gate,
):
    token_count, quarter = tokens.shape
    groups = lax.axis_size("grp")
    parts = lax.axis_size("tp")
    members = lax.axis_size("mem")
    capacity = token_count // 2
    share = capacity // parts
    slots = groups * capacity

    own = [w_gate[0], w_up[0], w_down[0]]
    across, other, diagonal = [], [], []
    for w in own:
        across.append(flip(w, "tp", 2))
        other.append(flip(w, "mem", 1))
    for i in range(2):
        diagonal.append(flip(across[i], "mem", 1))
    diagonal.append(flip(other[2], "tp", 2))
    sets = []
    for near, far in ((own, across), (other, diagonal)):
        near_pair = [flip(w, "tp", 1) for w in near]
        far_pair = [flip(w, "tp", 1) for w in far]
        sets.append([near, near_pair, far, far_pair])

    gain = norm_gain[None, :]
    far_gain = flip(gain, "tp", 2)
    gains = [gain, flip(gain, "tp", 1), far_gain, flip(far_gain, "tp", 1)]

    buffer, slot = pl.pallas_call(
        functools.partial(slots_kernel, groups=groups, members=members, parts=parts),
        out_shape=(
            jax.ShapeDtypeStruct((groups * parts, share + 8, quarter), jnp.bfloat16),
            jax.ShapeDtypeStruct((1, token_count), jnp.int32),
        ),
        in_specs=[VMEM] * 3,
        out_specs=(VMEM, VMEM),
        name="slots",
    )(routing.T, route_weight.T, tokens)
    arrived = lax.all_to_all(buffer, ("grp", "tp"), 0, 0, tiled=True)
    arrived = arrived.reshape(groups, parts, share + 8, quarter)

    total = groups * share
    normed, weights = pl.pallas_call(
        rows_kernel,
        out_shape=(
            jax.ShapeDtypeStruct((parts, total, quarter), jnp.bfloat16),
            jax.ShapeDtypeStruct((2, total, 1), jnp.float32),
        ),
        in_specs=[VMEM] * 5,
        out_specs=(VMEM, VMEM),
        name="rows",
    )(*gains, arrived)
    flat = [sets[e][k][m] for e in range(2) for m in range(2) for k in range(parts)]
    hidden = pl.pallas_call(
        hidden_kernel,
        out_shape=jax.ShapeDtypeStruct((2, total, own[0].shape[1]), jnp.bfloat16),
        in_specs=[VMEM] + [ANY] * len(flat),
        out_specs=VMEM,
        scratch_shapes=[
            pltpu.VMEM((len(flat),) + flat[0].shape, jnp.bfloat16),
            pltpu.SemaphoreType.DMA((len(flat),)),
        ],
        name="experts",
    )(normed, *flat)
    flat = [sets[e][k][2] for k in range(parts) for e in range(2)]
    results = pl.pallas_call(
        down_kernel,
        out_shape=jax.ShapeDtypeStruct((groups, parts, share, quarter), jnp.bfloat16),
        in_specs=[VMEM, VMEM] + [ANY] * len(flat),
        out_specs=VMEM,
        scratch_shapes=[
            pltpu.VMEM((len(flat),) + flat[0].shape, jnp.bfloat16),
            pltpu.SemaphoreType.DMA((len(flat),)),
        ],
        name="down",
    )(hidden, weights, *flat)
    returned = lax.all_to_all(
        results.reshape(groups * parts, share, quarter), ("grp", "tp"), 0, 0, tiled=True
    )

    far_tokens = flip(tokens, "tp", 2)
    token_parts = [tokens, flip(tokens, "tp", 1), far_tokens, flip(far_tokens, "tp", 1)]
    pieces = []
    for own_piece in (w_branch_in, w_branch_out):
        level = [own_piece]
        for k in range(1, groups):
            level.append(flip(own_piece, "grp", k))
        pieces += level
        for k in range(groups):
            pieces.append(flip(level[k], "mem", 1))
    piece = w_branch_in.shape
    wide = jax.ShapeDtypeStruct((token_count, quarter), jnp.float32)
    slim = jax.ShapeDtypeStruct((token_count, quarter), jnp.bfloat16)
    kept, near, held, far = pl.pallas_call(
        branch_kernel,
        out_shape=(wide, slim, wide, slim),
        in_specs=[VMEM] * 8 + [ANY] * len(pieces),
        out_specs=(VMEM,) * 4,
        scratch_shapes=[
            pltpu.VMEM((groups, 2) + piece, jnp.bfloat16),
            pltpu.VMEM((groups, 2) + w_branch_out.shape, jnp.bfloat16),
            pltpu.SemaphoreType.DMA((len(pieces),)),
        ],
        name="branch",
    )(*gains, *token_parts, *pieces)
    far = held + flip(far, "tp", 1).astype(jnp.float32)
    far = flip(far.astype(jnp.bfloat16), "tp", 2)
    near = flip(near, "tp", 1)
    return pl.pallas_call(
        finish_kernel,
        out_shape=jax.ShapeDtypeStruct((token_count, quarter), jnp.bfloat16),
        in_specs=[VMEM] * 6,
        out_specs=VMEM,
        name="finish",
    )(
        slot.reshape(token_count, 1),
        returned.reshape(slots, quarter),
        kept,
        near,
        far,
        branch_gate[None, :],
    )


def send_back(result):
    return lax.all_to_all(result, "ep", split_axis=0, concat_axis=0, tiled=True)


def body(
    tokens,
    norm_gain,
    routing,
    route_weight,
    w_gate,
    w_up,
    w_down,
    w_branch_in,
    w_branch_out,
    branch_gate,
):
    token_count, quarter = tokens.shape
    full_width = quarter * lax.axis_size("tp")
    floats = tokens.astype(jnp.float32)
    squares = lax.psum(jnp.sum(floats * floats, axis=1), "tp")
    normed = (floats * lax.rsqrt(squares[:, None] / full_width + epsilon) * norm_gain).astype(
        jnp.bfloat16
    )
    expert_count = lax.axis_size("ep") * w_gate.shape[0]
    capacity = token_count // (expert_count // GROUPS)
    flat_ids = routing.reshape(-1)
    one_hot = (flat_ids[:, None] == jnp.arange(expert_count, dtype=jnp.int32)[None, :]).astype(
        jnp.int32
    )
    before = jnp.cumsum(one_hot, axis=0) - one_hot
    position = flat_ids * capacity + jnp.sum(before * one_hot, axis=1)
    copies = jnp.repeat(normed, 2, axis=0)
    buffer = jnp.zeros((expert_count * capacity, quarter), jnp.bfloat16).at[position].set(copies)
    buffer = buffer.reshape(expert_count, capacity, quarter)
    gate_whole, up_whole, down_whole = (
        lax.all_gather(w_gate[0], "tp", axis=0, tiled=True),
        lax.all_gather(w_up[0], "tp", axis=0, tiled=True),
        lax.all_gather(w_down[0], "tp", axis=1, tiled=True),
    )
    row_split = lax.all_to_all(
        lax.all_to_all(buffer, "ep", split_axis=0, concat_axis=0, tiled=True),
        "tp",
        split_axis=0,
        concat_axis=2,
        tiled=True,
    )
    slot_rows = row_split.reshape(-1, row_split.shape[2])
    gate_sum = jnp.dot(slot_rows, gate_whole, preferred_element_type=jnp.float32)
    up_sum = jnp.dot(slot_rows, up_whole, preferred_element_type=jnp.float32)
    hidden = (jax.nn.silu(gate_sum) * up_sum).astype(jnp.bfloat16)
    result = jnp.dot(hidden, down_whole, preferred_element_type=jnp.float32).astype(jnp.bfloat16)
    feature_split = lax.all_to_all(
        result.reshape(row_split.shape), "tp", split_axis=2, concat_axis=0, tiled=True
    )
    returned = send_back(feature_split)
    picked = returned.reshape(expert_count * capacity, quarter)[position].reshape(
        token_count, 2, quarter
    )
    routed = jnp.sum(picked.astype(jnp.float32) * route_weight[:, :, None], axis=1)
    branch_tokens = lax.all_to_all(normed, "tp", split_axis=0, concat_axis=1, tiled=True)
    in_cols, out_rows = (
        lax.all_gather(w_branch_in, "tp", axis=1, tiled=True),
        lax.all_gather(w_branch_out, "tp", axis=0, tiled=True),
    )
    in_whole, out_whole = (
        lax.all_gather(in_cols, "ep", axis=0, tiled=True),
        lax.all_gather(out_rows, "ep", axis=1, tiled=True),
    )
    branch_hidden = jax.nn.silu(
        jnp.dot(branch_tokens, in_whole, preferred_element_type=jnp.float32)
    ).astype(jnp.bfloat16)
    branch_local = jnp.dot(branch_hidden, out_whole, preferred_element_type=jnp.float32).astype(
        jnp.bfloat16
    )
    branch = lax.all_to_all(branch_local, "tp", split_axis=1, concat_axis=0, tiled=True)
    return (routed + jax.nn.sigmoid(branch_gate) * branch.astype(jnp.float32)).astype(jnp.bfloat16)


def solution(mesh):
    shape = dict(mesh.shape)
    members = shape["ep"] // GROUPS
    paired = members == 2 and shape["tp"] == 4
    if paired:
        ep = ("grp", "mem")
        mesh = Mesh(
            mesh.devices.reshape(GROUPS, members, shape["tp"]), ("grp", "mem", "tp")
        )
    else:
        ep = "ep"
    return jax.shard_map(
        pair_body if paired else body,
        mesh=mesh,
        in_specs=(
            P(ep, "tp"),
            P("tp"),
            P(ep, None),
            P(ep, None),
            P(ep, "tp", None),
            P(ep, "tp", None),
            P(ep, None, "tp"),
            P(ep, "tp"),
            P("tp", ep),
            P("tp"),
        ),
        out_specs=P(ep, "tp"),
        check_vma=False,
    )
```
